32 devices in a mesh: sp: 4 (over z), fs: 4 (over y, x), tp: 2 (over core).
Axes of the slice: x: 2, y: 2, z: 4, core: 2. Of those that a mesh axis runs over, the one named last changes fastest.
Arguments:
- inputs: bfloat16 [4, 1024, 4096], P('fs', 'sp', 'tp'), may hold values from -6 to 6
- norm_gain: float32 [4096], replicated, may hold values from 0.1 to 1.9
- conv_in_a: bfloat16 [4096, 1024], P(('sp', 'fs'), 'tp'), may hold values from -0.09375 to 0.09375
- conv_in_b: bfloat16 [4096, 1024], P(('sp', 'fs'), 'tp'), may hold values from -0.09375 to 0.09375
- query_w: bfloat16 [4096, 512], P(('sp', 'fs'), 'tp'), may hold values from -0.09375 to 0.09375
- key_w: bfloat16 [4096, 512], P(('sp', 'fs'), 'tp'), may hold values from -0.09375 to 0.09375
- value_w: bfloat16 [4096, 1024], P(('sp', 'fs'), 'tp'), may hold values from -0.09375 to 0.09375
- out_gate_w: bfloat16 [4096, 1024], P(('sp', 'fs'), 'tp'), may hold values from -0.09375 to 0.09375
- pointwise_w: bfloat16 [4096, 1024], P(('sp', 'fs'), 'tp'), may hold values from -0.1875 to 0.1875
- gla_out_w: bfloat16 [4096, 1024], P(('sp', 'fs'), 'tp'), may hold values from -0.1875 to 0.1875
- forget_first_factor: bfloat16 [4096, 64], replicated, may hold values from -0.09375 to 0.09375
- decay_w: bfloat16 [64, 512], replicated, may hold values from -0.75 to 0.75
- decay_bias: float32 [512], replicated, as said below
- decay_extra: float32 [4, 1024, 512], P('fs', 'sp', 'tp'), may hold values from -2.2 to 0, as said below
- conv_kernel: float32 [31, 1024], replicated, may hold values from -7 to 7
- conv_gain: float32 [1024], replicated, may hold values from 0.1 to 1.9
- head_gain: float32 [64], replicated, may hold values from 0.1 to 1.9
Outputs:
- mixed: bfloat16 [4, 1024, 4096], P('fs', 'sp', 'tp')
The draws below stay inside these ranges and needn't reach their ends.
Inputs may be any that keep to these rules, and one draw needn't show every extreme that they name: decay_bias is positive. decay_extra is never positive.
All inputs are finite; a program needn't handle non-finite values.
Results may differ from the reference program's by a relative error of at most 0.015.
Values may be sent and summed in bfloat16 or wider, within the bound.
A program may use at most 192 MiB of HBM per device.

```python
import math
import jax
import jax.numpy as jnp
from jax import lax

D = 4096
C = 1024
GLA_HEADS = 16
DK = 32
DV = 64
RANK = 64
CONV_WIDTH = 31
BLOCK = 64
TOK_DEV = 256
SEQS = 4
LENGTH = 1024
HK = 512
HV = 1024
N_TP = 2


def draw_decay_bias(key, part):
    first_key = jax.random.fold_in(key, 11)
    second_key = jax.random.fold_in(key, 12)
    third_key = jax.random.fold_in(key, 13)
    slow_share = 0.5
    slow_heads = jax.random.bernoulli(first_key, slow_share, (GLA_HEADS,))
    slow_channels = jnp.repeat(slow_heads, DK)
    slow_value = math.log(LENGTH / 16.0) + jax.random.uniform(second_key, (HK,), jnp.float32, 1.0, 1.5)
    fast_value = jax.random.uniform(third_key, (HK,), jnp.float32, 0.5, 1.7)
    return jnp.where(slow_channels, slow_value, fast_value).astype(jnp.float32)


def draw_decay_extra(key, part):
    rate_key = jax.random.fold_in(key, 21)
    spot_key = jax.random.fold_in(key, 22)
    depth_key = jax.random.fold_in(key, 23)
    segment_count = LENGTH // TOK_DEV
    log_rate = jax.random.uniform(rate_key, (SEQS, segment_count, 1, HK), jnp.float32, math.log(0.15), math.log(0.6))
    forget_factors = jnp.broadcast_to(jnp.exp(log_rate) / LENGTH, (SEQS, segment_count, TOK_DEV, HK)).reshape(SEQS, LENGTH, HK)
    spots = jax.random.randint(spot_key, (SEQS, 3), 0, LENGTH)
    tier_heights = jax.random.uniform(depth_key, (SEQS, 3, HK), jnp.float32, math.log(0.5), math.log(0.8))
    agreement_tally = (jnp.arange(LENGTH, dtype=jnp.int32)[None, :, None] == spots[:, None, :]).astype(jnp.float32)
    spurt_sizes_list = jnp.einsum('dqz,dzc->dqc', agreement_tally, tier_heights)
    return (spurt_sizes_list - forget_factors).astype(jnp.float32)


def draw_conv_kernel(key, part):
    base_key = jax.random.fold_in(key, 31)
    base = jax.random.truncated_normal(base_key, -4.0, 4.0, (CONV_WIDTH, C), jnp.float32) * CONV_WIDTH ** (-0.5)
    rising = 3.0 ** (jnp.arange(C, dtype=jnp.float32) / (C - 1))
    return (base * rising).astype(jnp.float32)


def shard_levels(own_key, dims, shards, low, largest):
    level, own = 1.0, jax.random.fold_in(own_key, 6)
    for axis_at, parts in shards:
        heights = jnp.exp(jax.random.uniform(jax.random.fold_in(own, axis_at), (parts,), jnp.float32, low / len(shards), largest / len(shards)))
        level = level * jnp.repeat(heights, dims[axis_at] // parts).reshape([-1 if axis == axis_at else 1 for axis in range(len(dims))])
    return level


def normal_values(rng, extent, scale, limit, split=(), held_as=jnp.bfloat16):
    result = scale * jax.random.normal(rng, extent, jnp.float32)
    if split:
        result = result * shard_levels(rng, extent, split, -0.22, 0.18)
    return jnp.clip(result, -limit, limit).astype(held_as)


def setup_inputs(seed: int = 0) -> dict:
    key_of = jax.random.split(jax.random.key(seed), 18)
    inputs = normal_values(key_of[0], (SEQS, LENGTH, D), 1.0, 6.0, ((0, 4), (1, 4), (2, 2)))
    norm_gain = jnp.clip(1.0 + 0.18 * jax.random.normal(key_of[1], (D,), jnp.float32), 0.1, 1.9)
    conv_in_a = normal_values(key_of[2], (D, C), D ** -0.5, 0.09375, ((0, 16), (1, 2)))
    conv_in_b = normal_values(key_of[3], (D, C), D ** -0.5, 0.09375, ((0, 16), (1, 2)))
    query_w = normal_values(key_of[4], (D, HK), D ** -0.5, 0.09375, ((0, 16), (1, 2)))
    key_w = normal_values(key_of[5], (D, HK), D ** -0.5, 0.09375, ((0, 16), (1, 2)))
    value_w = normal_values(key_of[6], (D, HV), D ** -0.5, 0.09375, ((0, 16), (1, 2)))
    out_gate_w = normal_values(key_of[7], (D, HV), D ** -0.5, 0.09375, ((0, 16), (1, 2)))
    pointwise_w = normal_values(key_of[8], (D, C), C ** -0.5, 0.1875, ((0, 16), (1, 2)))
    gla_out_w = normal_values(key_of[9], (D, HV), HV ** -0.5, 0.1875, ((0, 16), (1, 2)))
    forget_first_factor = normal_values(key_of[10], (D, RANK), D ** -0.5, 0.09375)
    decay_w = normal_values(key_of[11], (RANK, HK), RANK ** -0.5, 0.75)
    decay_bias = draw_decay_bias(jax.random.fold_in(key_of[17], 71), 0)
    decay_extra = draw_decay_extra(jax.random.fold_in(key_of[17], 71), 0)
    conv_kernel = draw_conv_kernel(jax.random.fold_in(key_of[17], 71), 0)
    conv_gain = jnp.clip(1.0 + 0.18 * jax.random.normal(key_of[15], (C,), jnp.float32), 0.1, 1.9)
    head_gain = jnp.clip(1.0 + 0.18 * jax.random.normal(key_of[16], (DV,), jnp.float32), 0.1, 1.9)
    return dict(inputs=inputs, norm_gain=norm_gain, conv_in_a=conv_in_a, conv_in_b=conv_in_b, query_w=query_w, key_w=key_w, value_w=value_w, out_gate_w=out_gate_w, pointwise_w=pointwise_w, gla_out_w=gla_out_w, forget_first_factor=forget_first_factor, decay_w=decay_w, decay_bias=decay_bias, decay_extra=decay_extra, conv_kernel=conv_kernel, conv_gain=conv_gain, head_gain=head_gain)


def reference(inputs, norm_gain, conv_in_a, conv_in_b, query_w, key_w, value_w, out_gate_w, pointwise_w, gla_out_w, forget_first_factor, decay_w, decay_bias, decay_extra, conv_kernel, conv_gain, head_gain):
    position_count = SEQS * LENGTH
    flat_rows = inputs.reshape(position_count, D).astype(jnp.float32)
    row_scale = lax.rsqrt(lax.optimization_barrier(jnp.mean(flat_rows * flat_rows, axis=1, keepdims=True)) + 1e-06)
    scaled = (flat_rows * norm_gain).astype(jnp.bfloat16)

    def project(weight):
        product = jnp.dot(scaled, weight, preferred_element_type=jnp.float32)
        return (product * row_scale).astype(jnp.bfloat16)
    conv_a, conv_b, queries, keys, values, out_gate, low_rank = [project(weight) for weight in (conv_in_a, conv_in_b, query_w, key_w, value_w, out_gate_w, forget_first_factor)]
    gated = (conv_a.astype(jnp.float32) * jax.nn.sigmoid(conv_b.astype(jnp.float32))).astype(jnp.bfloat16)
    padded = jnp.pad(gated.reshape(SEQS, LENGTH, C).astype(jnp.float32), ((0, 0), (CONV_WIDTH - 1, 0), (0, 0)))
    convolved = jnp.zeros((SEQS, LENGTH, C), jnp.float32)
    for offset in range(CONV_WIDTH):
        convolved = convolved + conv_kernel[offset] * padded[:, offset:offset + LENGTH]
    average = lax.optimization_barrier(jnp.mean(convolved, axis=-1, keepdims=True))
    spread_squared_mean = lax.optimization_barrier(jnp.mean(jnp.square(convolved - average), axis=-1, keepdims=True))
    normed = (convolved - average) * lax.rsqrt(spread_squared_mean + 1e-05) * conv_gain
    conv_act = jax.nn.silu(normed).astype(jnp.bfloat16).reshape(position_count, C)
    pre_decay = jnp.dot(low_rank, decay_w, preferred_element_type=jnp.float32) + decay_bias
    log_decay = jax.nn.log_sigmoid(pre_decay) / 16.0 + decay_extra.reshape(position_count, HK)
    block_count = LENGTH // BLOCK

    def split_blocks(array_operand, width):
        return array_operand.reshape(SEQS, block_count, BLOCK, GLA_HEADS, width).transpose(1, 0, 3, 2, 4)
    q_blocks = split_blocks(queries.astype(jnp.float32), DK) * DK ** (-0.5)
    k_blocks = split_blocks(keys.astype(jnp.float32), DK)
    v_blocks = split_blocks(values.astype(jnp.float32), DV)
    cumulative_all = jnp.cumsum(split_blocks(log_decay, DK), axis=3)
    causal = jnp.tril(jnp.ones((BLOCK, BLOCK), dtype=bool))
    highest = lax.Precision.HIGHEST

    def advance(state, block_inputs):
        query_block, key_block, value_block, prefix_running_sum = block_inputs
        spread = prefix_running_sum[..., :, None, :] - prefix_running_sum[..., None, :, :]
        weights_in = jnp.exp(jnp.where(causal[:, :, None], spread, -jnp.inf))
        scores = jnp.einsum('shid,shjd,shijd->shij', query_block, key_block, weights_in, precision=highest)
        inner = jnp.einsum('shij,shjv->shiv', scores, value_block, precision=highest)
        outer = jnp.einsum('shid,shdv->shiv', query_block * jnp.exp(prefix_running_sum), state, precision=highest)
        last_total = prefix_running_sum[..., -1, :]
        added_share_term = jnp.einsum('shjd,shjv->shdv', key_block * jnp.exp(last_total[..., None, :] - prefix_running_sum), value_block, precision=highest)
        return (jnp.exp(last_total)[..., None] * state + added_share_term, inner + outer)
    start_state = jnp.zeros((SEQS, GLA_HEADS, DK, DV), jnp.float32)
    _, outputs = lax.scan(advance, start_state, (q_blocks, k_blocks, v_blocks, cumulative_all))
    outputs = outputs.transpose(1, 0, 3, 2, 4).reshape(position_count, GLA_HEADS, DV)
    normed_heads = outputs * lax.rsqrt(lax.optimization_barrier(jnp.mean(outputs * outputs, axis=-1, keepdims=True)) + 1e-06) * head_gain
    gla_act = (normed_heads.reshape(position_count, HV) * jax.nn.silu(out_gate.astype(jnp.float32))).astype(jnp.bfloat16)
    conv_group = C // N_TP
    head_group = HV // N_TP
    total = flat_rows
    for group_index in range(N_TP):
        convolution_window = slice(group_index * conv_group, (group_index + 1) * conv_group)
        head_slice = slice(group_index * head_group, (group_index + 1) * head_group)
        value_fraction = jnp.dot(conv_act[:, convolution_window], pointwise_w[:, convolution_window].T, preferred_element_type=jnp.float32)
        value_fraction = value_fraction + jnp.dot(gla_act[:, head_slice], gla_out_w[:, head_slice].T, preferred_element_type=jnp.float32)
        total = total + lax.optimization_barrier(value_fraction.astype(jnp.bfloat16)).astype(jnp.float32)
    return total.astype(jnp.bfloat16).reshape(SEQS, LENGTH, D)
```

```python
import functools

import jax
import jax.numpy as jnp
from jax import lax
from jax.experimental import pallas as pl
from jax.experimental.pallas import tpu as pltpu
from jax.sharding import PartitionSpec as P

DK = 32
DV = 64
SUB = 16
BLOCK = 64


def gla_kernel(q_ref, k_ref, v_ref, g_ref, ld_ref, hg_ref, o_ref, state_ref, *, rows, chunk):
    kw = q_ref.shape[1]
    vw = v_ref.shape[1]
    f32, bf16 = jnp.float32, jnp.bfloat16
    spread = (
        lax.broadcasted_iota(jnp.int32, (kw, vw), 0) // DK
        == lax.broadcasted_iota(jnp.int32, (kw, vw), 1) // DV
    ).astype(bf16)
    own = (
        lax.broadcasted_iota(jnp.int32, (vw, kw), 1) // DK
        == lax.broadcasted_iota(jnp.int32, (vw, kw), 0) // DV
    )
    head_mean = jnp.where(
        lax.broadcasted_iota(jnp.int32, (vw, vw), 0) // DV
        == lax.broadcasted_iota(jnp.int32, (vw, vw), 1) // DV,
        1.0 / DV,
        0.0,
    ).astype(f32)
    state_ref[...] = jnp.zeros_like(state_ref)
    place = lax.broadcasted_iota(jnp.int32, (chunk, kw), 0) % SUB

    def body(n, carry):
        at = pl.ds(pl.multiple_of(n * chunk, chunk), chunk)
        q = q_ref[at, :].astype(f32) * DK ** (-0.5)
        k = k_ref[at, :].astype(f32)
        v = v_ref[at, :].astype(f32)
        cum = ld_ref[at, :]
        step = 1
        while step < SUB:
            cum = cum + jnp.where(place >= step, pltpu.roll(cum, step, 0), 0.0)
            step *= 2
        acc = jnp.dot((q * k).astype(bf16), spread, preferred_element_type=f32) * v
        for lag in range(1, SUB):
            decay = jnp.exp(jnp.where(place >= lag, cum - pltpu.roll(cum, lag, 0), -jnp.inf))
            term = (q * pltpu.roll(k, lag, 0) * decay).astype(bf16)
            score = jnp.dot(term, spread, preferred_element_type=f32)
            acc = acc + score * pltpu.roll(v, lag, 0)
        q_in = (q * jnp.exp(cum)).astype(bf16)
        v_low = v.astype(bf16)
        state = state_ref[...]
        outer = []
        for m in range(chunk // SUB):
            part = slice(m * SUB, (m + 1) * SUB)
            total = cum[(m + 1) * SUB - 1 : (m + 1) * SUB]
            k_out = (k[part] * jnp.exp(total - cum[part])).astype(bf16)
            outer.append(
                lax.dot_general(
                    q_in[part], state.astype(bf16), (((1,), (1,)), ((), ())),
                    preferred_element_type=f32,
                )
            )
            added = lax.dot_general(
                v_low[part], k_out, (((0,), (0,)), ((), ())), preferred_element_type=f32
            )
            state = state * jnp.exp(total) + jnp.where(own, added, 0.0)
        state_ref[...] = state
        raw = acc + jnp.concatenate(outer, axis=0)
        mean = jnp.dot(
            raw * raw, head_mean, preferred_element_type=f32, precision=lax.Precision.HIGHEST
        )
        gate = g_ref[at, :].astype(f32)
        o_ref[at, :] = (
            raw * lax.rsqrt(mean + 1e-06) * hg_ref[...] * (gate * jax.nn.sigmoid(gate))
        ).astype(o_ref.dtype)
        return carry

    lax.fori_loop(0, rows // chunk, body, 0)


def gla(queries, keys, values, gate, log_decay, gain):
    rows, kw = queries.shape
    vw = values.shape[1]
    return pl.pallas_call(
        functools.partial(gla_kernel, rows=rows, chunk=128),
        out_shape=jax.ShapeDtypeStruct((rows, vw), jnp.bfloat16),
        in_specs=[pl.BlockSpec(memory_space=pltpu.VMEM)] * 6,
        out_specs=pl.BlockSpec(memory_space=pltpu.VMEM),
        scratch_shapes=[pltpu.VMEM((vw, kw), jnp.float32)],
        cost_estimate=pl.CostEstimate(
            flops=40_000_000_000, bytes_accessed=4_000_000, transcendentals=2_000_000
        ),
        name="gla",
    )(queries, keys, values, gate, log_decay, gain)


def spread_columns(weights, count):
    return jnp.concatenate(
        [w.reshape(w.shape[0], count, w.shape[1] // count) for w in weights], axis=2
    ).transpose(1, 0, 2)


def by_heads(
    inputs,
    norm_gain,
    conv_in_a,
    conv_in_b,
    query_w,
    key_w,
    value_w,
    out_gate_w,
    pointwise_w,
    gla_out_w,
    forget_first_factor,
    decay_w,
    decay_bias,
    decay_extra,
    conv_kernel,
    conv_gain,
    head_gain,
):
    bf16, f32 = jnp.bfloat16, jnp.float32
    n_sp = lax.axis_size("sp")
    n_tp = lax.axis_size("tp")
    n_fs = lax.axis_size("fs")
    sp, tp = lax.axis_index("sp"), lax.axis_index("tp")
    tokens = inputs.shape[1]
    length = n_sp * tokens
    own_rows = inputs[0]
    in_weights = (conv_in_a, conv_in_b, query_w, key_w, value_w, out_gate_w)
    widths = [w.shape[1] // n_sp for w in in_weights]
    chunks = lax.all_to_all(spread_columns(in_weights, n_sp), "sp", 0, 0)
    rows = chunks.shape[1]
    in_full = lax.all_gather(chunks, "fs", axis=1).reshape(n_sp * n_fs * rows, sum(widths))
    out_local = jnp.concatenate([pointwise_w, gla_out_w], axis=1)
    out_full = lax.all_gather(out_local, "fs", axis=0, tiled=True)
    half = lax.all_gather(own_rows, "sp", axis=0, tiled=True)
    x = lax.all_gather(half, "tp", axis=1, tiled=True)
    features = x.shape[1]
    xf = x.astype(f32)
    row_scale = lax.rsqrt(jnp.sum(xf * xf, axis=1) / features + 1e-06)[:, None]
    scaled = (xf * norm_gain).astype(bf16)

    product = jnp.dot(scaled, in_full, preferred_element_type=f32)
    product = (product * row_scale).astype(bf16)
    at, parts = 0, []
    for width in widths:
        parts.append(product[:, at : at + width])
        at += width
    conv_a, conv_b, queries, keys, values, out_gate = parts
    low_rank = (
        jnp.dot(scaled, forget_first_factor, preferred_element_type=f32) * row_scale
    ).astype(bf16)

    gated = (conv_a.astype(f32) * jax.nn.sigmoid(conv_b.astype(f32))).astype(bf16)
    channels = gated.shape[1]
    taps = conv_kernel.shape[0]
    first = (tp * n_sp + sp) * channels
    kernel = lax.dynamic_slice_in_dim(conv_kernel, first, channels, 1)
    extended = jnp.pad(gated.astype(f32), ((taps - 1, 0), (0, 0)))
    convolved = jnp.zeros((length, channels), f32)
    for offset in range(taps):
        convolved = convolved + kernel[offset] * extended[offset : offset + length]
    stats = lax.psum(
        jnp.stack([jnp.sum(convolved, axis=1), jnp.sum(convolved * convolved, axis=1)]),
        ("sp", "tp"),
    )
    total = conv_gain.shape[0]
    average = stats[0] / total
    variance = stats[1] / total - average * average
    gain_part = lax.dynamic_slice_in_dim(conv_gain, first, channels)
    normed = (convolved - average[:, None]) * lax.rsqrt(variance + 1e-05)[:, None] * gain_part
    conv_act = jax.nn.silu(normed).astype(bf16)

    key_width = keys.shape[1]
    first_key = (tp * n_sp + sp) * key_width
    decay_part = lax.dynamic_slice_in_dim(decay_w, first_key, key_width, 1)
    bias_part = lax.dynamic_slice_in_dim(decay_bias, first_key, key_width)
    extra = decay_extra[0].reshape(tokens, n_sp, key_width).transpose(1, 0, 2)
    extra = lax.all_to_all(extra, "sp", 0, 0).reshape(length, key_width)
    pre_decay = jnp.dot(low_rank, decay_part, preferred_element_type=f32) + bias_part
    log_decay = jax.nn.log_sigmoid(pre_decay) / 16.0 + extra
    gains = jnp.tile(head_gain, key_width // DK)[None]
    gla_act = gla(queries, keys, values, out_gate, log_decay, gains)

    acts = jnp.stack([conv_act, gla_act])
    acts = lax.all_gather(acts, "sp", axis=0)
    acts = acts.transpose(2, 1, 0, 3).reshape(length, 2 * n_sp * channels)
    partial = lax.dot_general(
        acts, out_full, (((1,), (1,)), ((), ())), preferred_element_type=f32
    ).astype(bf16)
    partial = partial.reshape(n_sp, tokens, partial.shape[1])
    partial = lax.all_to_all(partial, "sp", 0, 0)
    partial = partial.reshape(n_tp, n_sp // n_tp, tokens, partial.shape[2])
    summed = lax.psum_scatter(partial, "tp", scatter_dimension=0, tiled=False)
    summed = summed.transpose(1, 0, 2).reshape(tokens, own_rows.shape[1])
    return (own_rows.astype(f32) + summed.astype(f32)).astype(bf16)[None]


def from_behind(value, axis, by):
    length = lax.axis_size(axis)
    pairs = [(i, i + by) for i in range(length) if 0 <= i + by < length]
    return lax.ppermute(value, axis, pairs)


def by_tokens(
    inputs,
    norm_gain,
    conv_in_a,
    conv_in_b,
    query_w,
    key_w,
    value_w,
    out_gate_w,
    pointwise_w,
    gla_out_w,
    forget_first_factor,
    decay_w,
    decay_bias,
    decay_extra,
    conv_kernel,
    conv_gain,
    head_gain,
):
    collected = (
        lax.all_gather(conv_in_a, ("sp", "fs"), axis=0, tiled=True),
        lax.all_gather(conv_in_b, ("sp", "fs"), axis=0, tiled=True),
        lax.all_gather(query_w, ("sp", "fs"), axis=0, tiled=True),
        lax.all_gather(key_w, ("sp", "fs"), axis=0, tiled=True),
        lax.all_gather(value_w, ("sp", "fs"), axis=0, tiled=True),
        lax.all_gather(out_gate_w, ("sp", "fs"), axis=0, tiled=True),
        lax.all_gather(pointwise_w, ("sp", "fs"), axis=0, tiled=True),
        lax.all_gather(gla_out_w, ("sp", "fs"), axis=0, tiled=True),
    )
    (
        conv_a_full,
        conv_b_full,
        query_full,
        key_full,
        value_full,
        gate_full,
        pointwise_full,
        gla_out_full,
    ) = collected
    tok_rows = inputs[0]
    token_count = tok_rows.shape[0]
    in_weights = (
        conv_a_full,
        conv_b_full,
        query_full,
        key_full,
        value_full,
        gate_full,
        forget_first_factor,
    )
    segment_values = lax.all_gather(tok_rows, "tp", axis=1, tiled=True).astype(jnp.float32)
    scaled = (segment_values * norm_gain).astype(jnp.bfloat16)
    sums = tuple(
        (jnp.dot(scaled, weight, preferred_element_type=jnp.float32) for weight in in_weights)
    )
    sums, squares = (sums, jnp.sum(segment_values * segment_values, axis=1))
    row_scale = lax.rsqrt(squares / norm_gain.shape[0] + 1e-06)[:, None]
    conv_a, conv_b, queries, keys, values, out_gate, low_rank = [
        (running * row_scale).astype(jnp.bfloat16) for running in sums
    ]
    gated = (conv_a.astype(jnp.float32) * jax.nn.sigmoid(conv_b.astype(jnp.float32))).astype(
        jnp.bfloat16
    )
    reach = conv_kernel.shape[0] - 1
    earlier = from_behind(gated[token_count - reach :], "sp", 1)
    extended = jnp.concatenate([earlier, gated], axis=0).astype(jnp.float32)
    tp_index = lax.axis_index("tp")
    channels = gated.shape[1]
    kernel = lax.dynamic_slice_in_dim(conv_kernel, tp_index * channels, channels, 1)
    convolved = jnp.zeros((token_count, channels), jnp.float32)
    for offset in range(reach + 1):
        convolved = convolved + kernel[offset] * extended[offset : offset + token_count]
    channel_sum, channel_squares = lax.psum(
        (jnp.sum(convolved, axis=1), jnp.sum(convolved * convolved, axis=1)), "tp"
    )
    total_channels = conv_gain.shape[0]
    average = channel_sum / total_channels
    spread_squared_mean = channel_squares / total_channels - average * average
    gain_part = lax.dynamic_slice_in_dim(conv_gain, tp_index * channels, channels)
    normed = (
        (convolved - average[:, None]) * lax.rsqrt(spread_squared_mean + 1e-05)[:, None] * gain_part
    )
    conv_act = jax.nn.silu(normed).astype(jnp.bfloat16)
    key_width = keys.shape[1]
    head_count = key_width // DK
    decay_part = lax.dynamic_slice_in_dim(decay_w, tp_index * key_width, key_width, 1)
    bias_part = lax.dynamic_slice_in_dim(decay_bias, tp_index * key_width, key_width)
    pre_decay = jnp.dot(low_rank, decay_part, preferred_element_type=jnp.float32) + bias_part
    log_decay = jax.nn.log_sigmoid(pre_decay) / 16.0 + decay_extra[0]
    block_count = token_count // BLOCK
    highest = lax.Precision.HIGHEST

    def split_blocks(array_operand, width):
        return array_operand.reshape(block_count, BLOCK, head_count, width).transpose(0, 2, 1, 3)

    q_blocks = split_blocks(queries.astype(jnp.float32), DK) * DK ** (-0.5)
    k_blocks = split_blocks(keys.astype(jnp.float32), DK)
    v_blocks = split_blocks(values.astype(jnp.float32), DV)
    prefix_running_sum = jnp.cumsum(split_blocks(log_decay, DK), axis=2)
    causal = jnp.tril(jnp.ones((BLOCK, BLOCK), dtype=bool))
    spread = prefix_running_sum[:, :, :, None, :] - prefix_running_sum[:, :, None, :, :]
    weights_in = jnp.exp(jnp.where(causal[:, :, None], spread, -jnp.inf))
    scores = jnp.einsum("nhid,nhjd,nhijd->nhij", q_blocks, k_blocks, weights_in, precision=highest)
    inner = jnp.einsum("nhij,nhjv->nhiv", scores, v_blocks, precision=highest)
    block_total = prefix_running_sum[:, :, -1]
    block_state = jnp.einsum(
        "nhjd,nhjv->nhdv",
        k_blocks * jnp.exp(block_total[:, :, None] - prefix_running_sum),
        v_blocks,
        precision=highest,
    )

    def advance(state, block_pair):
        decay_row, added_share_term = block_pair
        return (jnp.exp(decay_row)[..., None] * state + added_share_term, state)

    local_final, local_entering = lax.scan(
        advance, jnp.zeros((head_count, DK, DV), jnp.float32), (block_total, block_state)
    )
    device_total = jnp.sum(block_total, axis=0)
    totals = lax.all_gather(device_total[None], "sp", axis=0, tiled=True)
    running_totals = jnp.cumsum(totals, axis=0)
    sp_index = lax.axis_index("sp")
    before = lax.dynamic_index_in_dim(
        running_totals, sp_index, 0, False
    ) - lax.dynamic_index_in_dim(totals, sp_index, 0, False)
    piece = lax.all_gather(local_final[None], "sp", axis=0, tiled=True)
    number = piece.shape[0]
    anchor = jnp.arange(number, dtype=jnp.int32)
    exponent = jnp.where(
        (anchor < sp_index)[:, None, None], before[None] - running_totals, -jnp.inf
    )
    entering = jnp.einsum("nhd,nhdv->hdv", jnp.exp(exponent), piece, precision=highest)
    passed = jnp.exp(jnp.cumsum(block_total, axis=0) - block_total)
    entering_blocks = passed[..., None] * entering[None] + local_entering
    outer = jnp.einsum(
        "nhid,nhdv->nhiv",
        q_blocks * jnp.exp(prefix_running_sum),
        entering_blocks,
        precision=highest,
    )
    head_output = inner + outer
    normed_heads = (
        head_output
        * lax.rsqrt(jnp.mean(head_output * head_output, axis=-1, keepdims=True) + 1e-06)
        * head_gain
    )
    gla_rows = normed_heads.transpose(0, 2, 1, 3).reshape(token_count, head_count * DV)
    gla_act = (gla_rows * jax.nn.silu(out_gate.astype(jnp.float32))).astype(jnp.bfloat16)
    contract = (((1,), (1,)), ((), ()))
    conv_term = lax.dot_general(
        pointwise_full, conv_act, contract, preferred_element_type=jnp.float32
    )
    summed = lax.psum_scatter(
        (
            conv_term
            + lax.dot_general(gla_out_full, gla_act, contract, preferred_element_type=jnp.float32)
        ).astype(jnp.bfloat16),
        "tp",
        scatter_dimension=0,
        tiled=True,
    ).astype(jnp.float32)
    return (tok_rows.astype(jnp.float32) + summed.T).astype(jnp.bfloat16)[None]


def shards(*args):
    n_sp, n_tp = lax.axis_size("sp"), lax.axis_size("tp")
    head_count = args[5].shape[1] // DK
    whole_heads = head_count % n_sp == 0 and n_sp % n_tp == 0
    return by_heads(*args) if whole_heads else by_tokens(*args)


def solution(mesh):
    by_rows = P(("sp", "fs"), "tp")
    return jax.shard_map(
        shards,
        mesh=mesh,
        in_specs=(P("fs", "sp", "tp"), P())
        + (by_rows,) * 8
        + (P(), P(), P(), P("fs", "sp", "tp"), P(), P(), P()),
        out_specs=P("fs", "sp", "tp"),
        check_vma=False,
    )
```

```python
import functools

import jax
import jax.numpy as jnp
from jax import lax
from jax.experimental import pallas as pl
from jax.experimental.pallas import tpu as pltpu
from jax.sharding import PartitionSpec as P


DK = 32
DV = 64
SUB = 16
BLOCK = 64


def gla_kernel(q_ref, k_ref, v_ref, g_ref, ld_ref, hg_ref, o_ref, state_ref, *, rows, chunk):
    kw = q_ref.shape[1]
    vw = v_ref.shape[1]
    f32, bf16 = jnp.float32, jnp.bfloat16
    spread = (
        lax.broadcasted_iota(jnp.int32, (kw, vw), 0) // DK
        == lax.broadcasted_iota(jnp.int32, (kw, vw), 1) // DV
    ).astype(bf16)
    own = (
        lax.broadcasted_iota(jnp.int32, (vw, kw), 1) // DK
        == lax.broadcasted_iota(jnp.int32, (vw, kw), 0) // DV
    )
    head_mean = jnp.where(
        lax.broadcasted_iota(jnp.int32, (vw, vw), 0) // DV
        == lax.broadcasted_iota(jnp.int32, (vw, vw), 1) // DV,
        1.0 / DV,
        0.0,
    ).astype(f32)
    state_ref[...] = jnp.zeros_like(state_ref)
    place = lax.broadcasted_iota(jnp.int32, (chunk, kw), 0) % SUB

    def body(n, carry):
        at = pl.ds(pl.multiple_of(n * chunk, chunk), chunk)
        q = q_ref[at, :].astype(f32) * DK ** (-0.5)
        k = k_ref[at, :].astype(f32)
        v = v_ref[at, :].astype(f32)
        cum = ld_ref[at, :]
        step = 1
        while step < SUB:
            cum = cum + jnp.where(place >= step, pltpu.roll(cum, step, 0), 0.0)
            step *= 2
        acc = jnp.dot((q * k).astype(bf16), spread, preferred_element_type=f32) * v
        for lag in range(1, SUB):
            decay = jnp.exp(jnp.where(place >= lag, cum - pltpu.roll(cum, lag, 0), -jnp.inf))
            term = (q * pltpu.roll(k, lag, 0) * decay).astype(bf16)
            score = jnp.dot(term, spread, preferred_element_type=f32)
            acc = acc + score * pltpu.roll(v, lag, 0)
        q_in = (q * jnp.exp(cum)).astype(bf16)
        v_low = v.astype(bf16)
        state = state_ref[...]
        outer = []
        for m in range(chunk // SUB):
            part = slice(m * SUB, (m + 1) * SUB)
            total = cum[(m + 1) * SUB - 1 : (m + 1) * SUB]
            k_out = (k[part] * jnp.exp(total - cum[part])).astype(bf16)
            outer.append(
                lax.dot_general(
                    q_in[part], state.astype(bf16), (((1,), (1,)), ((), ())),
                    preferred_element_type=f32,
                )
            )
            added = lax.dot_general(
                v_low[part], k_out, (((0,), (0,)), ((), ())), preferred_element_type=f32
            )
            state = state * jnp.exp(total) + jnp.where(own, added, 0.0)
        state_ref[...] = state
        raw = acc + jnp.concatenate(outer, axis=0)
        mean = jnp.dot(
            raw * raw, head_mean, preferred_element_type=f32, precision=lax.Precision.HIGHEST
        )
        gate = g_ref[at, :].astype(f32)
        o_ref[at, :] = (
            raw * lax.rsqrt(mean + 1e-06) * hg_ref[...] * (gate * jax.nn.sigmoid(gate))
        ).astype(o_ref.dtype)
        return carry

    lax.fori_loop(0, rows // chunk, body, 0)


def gla(queries, keys, values, gate, log_decay, gain):
    rows, kw = queries.shape
    vw = values.shape[1]
    return pl.pallas_call(
        functools.partial(gla_kernel, rows=rows, chunk=128),
        out_shape=jax.ShapeDtypeStruct((rows, vw), jnp.bfloat16),
        in_specs=[pl.BlockSpec(memory_space=pltpu.VMEM)] * 6,
        out_specs=pl.BlockSpec(memory_space=pltpu.VMEM),
        scratch_shapes=[pltpu.VMEM((vw, kw), jnp.float32)],
        cost_estimate=pl.CostEstimate(
            flops=40_000_000_000, bytes_accessed=4_000_000, transcendentals=2_000_000
        ),
        name="gla",
    )(queries, keys, values, gate, log_decay, gain)


def spread_columns(weights, count):
    return jnp.concatenate(
        [w.reshape(w.shape[0], count, w.shape[1] // count) for w in weights], axis=2
    ).transpose(1, 0, 2)


def exchange_chunks(chunks, count):
    me = lax.axis_index("sp")
    got = [lax.dynamic_index_in_dim(chunks, me, 0, False)]
    for shift in range(1, count):
        piece = lax.dynamic_index_in_dim(chunks, (me + shift) % count, 0, False)
        got.append(lax.ppermute(piece, "sp", [(i, (i + shift) % count) for i in range(count)]))
    ordered = jnp.stack([got[-q % count] for q in range(count)] * 2)
    return lax.dynamic_slice_in_dim(ordered, -me % count, count, 0)


def chain_gather(block, count):
    rows = block.shape[0]
    up = [(i, i + 1) for i in range(count - 1)]
    down = [(i + 1, i) for i in range(count - 1)]
    below, above = [block], [block]
    for _ in range(count - 1):
        below.append(lax.ppermute(below[-1], "sp", up))
        above.append(lax.ppermute(above[-1], "sp", down))
    line = jnp.concatenate(below[:0:-1] + above, axis=0)
    start = (count - 1 - lax.axis_index("sp")) * rows
    return lax.dynamic_slice_in_dim(line, start, count * rows, 0)


def by_heads(
    inputs,
    norm_gain,
    conv_in_a,
    conv_in_b,
    query_w,
    key_w,
    value_w,
    out_gate_w,
    pointwise_w,
    gla_out_w,
    forget_first_factor,
    decay_w,
    decay_bias,
    decay_extra,
    conv_kernel,
    conv_gain,
    head_gain,
):
    bf16, f32 = jnp.bfloat16, jnp.float32
    n_sp = lax.axis_size("sp")
    n_tp = lax.axis_size("tp")
    n_fs = lax.axis_size("fs")
    sp, tp = lax.axis_index("sp"), lax.axis_index("tp")
    tokens = inputs.shape[1]
    length = n_sp * tokens
    own_rows = inputs[0]
    in_weights = (conv_in_a, conv_in_b, query_w, key_w, value_w, out_gate_w)
    widths = [w.shape[1] // n_sp for w in in_weights]
    chunks = exchange_chunks(spread_columns(in_weights, n_sp), n_sp)
    chunks, sent_rows = lax.optimization_barrier((chunks, own_rows))
    rows = chunks.shape[1]
    in_full = lax.all_gather(chunks, "fs", axis=1).reshape(n_sp * n_fs * rows, sum(widths))
    out_local = jnp.concatenate([pointwise_w, gla_out_w], axis=1)
    half = chain_gather(sent_rows, n_sp)
    x = lax.all_gather(half, "tp", axis=1, tiled=True)
    out_local, x = lax.optimization_barrier((out_local, x))
    out_full = lax.all_gather(out_local, "fs", axis=0, tiled=True)
    features = x.shape[1]
    xf = x.astype(f32)
    row_scale = lax.rsqrt(jnp.sum(xf * xf, axis=1) / features + 1e-06)[:, None]
    scaled = (xf * norm_gain).astype(bf16)

    product = jnp.dot(scaled, in_full, preferred_element_type=f32)
    product = (product * row_scale).astype(bf16)
    at, parts = 0, []
    for width in widths:
        parts.append(product[:, at : at + width])
        at += width
    conv_a, conv_b, queries, keys, values, out_gate = parts
    low_rank = (
        jnp.dot(scaled, forget_first_factor, preferred_element_type=f32) * row_scale
    ).astype(bf16)

    gated = (conv_a.astype(f32) * jax.nn.sigmoid(conv_b.astype(f32))).astype(bf16)
    channels = gated.shape[1]
    taps = conv_kernel.shape[0]
    first = (tp * n_sp + sp) * channels
    kernel = lax.dynamic_slice_in_dim(conv_kernel, first, channels, 1)
    extended = jnp.pad(gated.astype(f32), ((taps - 1, 0), (0, 0)))
    convolved = jnp.zeros((length, channels), f32)
    for offset in range(taps):
        convolved = convolved + kernel[offset] * extended[offset : offset + length]
    stats = lax.psum(
        jnp.stack([jnp.sum(convolved, axis=1), jnp.sum(convolved * convolved, axis=1)]),
        ("sp", "tp"),
    )
    total = conv_gain.shape[0]
    average = stats[0] / total
    variance = stats[1] / total - average * average
    gain_part = lax.dynamic_slice_in_dim(conv_gain, first, channels)
    normed = (convolved - average[:, None]) * lax.rsqrt(variance + 1e-05)[:, None] * gain_part
    conv_act = jax.nn.silu(normed).astype(bf16)

    key_width = keys.shape[1]
    first_key = (tp * n_sp + sp) * key_width
    decay_part = lax.dynamic_slice_in_dim(decay_w, first_key, key_width, 1)
    bias_part = lax.dynamic_slice_in_dim(decay_bias, first_key, key_width)
    extra = decay_extra[0].reshape(tokens, n_sp, key_width).transpose(1, 0, 2)
    extra = lax.all_to_all(extra, "sp", 0, 0).reshape(length, key_width)
    pre_decay = jnp.dot(low_rank, decay_part, preferred_element_type=f32) + bias_part
    log_decay = jax.nn.log_sigmoid(pre_decay) / 16.0 + extra
    gains = jnp.tile(head_gain, key_width // DK)[None]
    gla_act = gla(queries, keys, values, out_gate, log_decay, gains)

    conv_act, out_full = lax.optimization_barrier((conv_act, out_full))
    conv_all = lax.all_gather(conv_act, "sp", axis=0)
    gla_act, conv_all = lax.optimization_barrier((gla_act, conv_all))
    gla_all = lax.all_gather(gla_act, "sp", axis=0)

    def project(gathered, weight):
        merged = gathered.transpose(1, 0, 2).reshape(length, n_sp * channels)
        return lax.dot_general(
            merged, weight, (((1,), (1,)), ((), ())), preferred_element_type=f32
        )

    width = n_sp * channels
    partial = project(conv_all, out_full[:, :width]) + project(gla_all, out_full[:, width:])
    summed = lax.psum_scatter(
        partial.astype(bf16), "tp", scatter_dimension=0, tiled=True
    )
    share = n_sp // n_tp
    summed = summed.reshape(share, tokens, summed.shape[1])
    got = []
    for turn in range(share):
        piece = lax.dynamic_index_in_dim(summed, (turn + sp) % share, 0, False)
        pairs = [
            (k * n_tp + t, (t * share + (turn + k) % share) * n_tp + k // share)
            for k in range(n_sp)
            for t in range(n_tp)
        ]
        got.append(lax.ppermute(piece, ("sp", "tp"), pairs))
    ordered = jnp.stack([got[-q % share] for q in range(share)] * 2)
    ordered = lax.dynamic_slice_in_dim(ordered, -sp % share, share, 0)
    summed = ordered.transpose(1, 0, 2).reshape(tokens, own_rows.shape[1])
    return (own_rows.astype(f32) + summed.astype(f32)).astype(bf16)[None]


def from_behind(value, axis, by):
    length = lax.axis_size(axis)
    pairs = [(i, i + by) for i in range(length) if 0 <= i + by < length]
    return lax.ppermute(value, axis, pairs)


def by_tokens(
    inputs,
    norm_gain,
    conv_in_a,
    conv_in_b,
    query_w,
    key_w,
    value_w,
    out_gate_w,
    pointwise_w,
    gla_out_w,
    forget_first_factor,
    decay_w,
    decay_bias,
    decay_extra,
    conv_kernel,
    conv_gain,
    head_gain,
):
    collected = (
        lax.all_gather(conv_in_a, ("sp", "fs"), axis=0, tiled=True),
        lax.all_gather(conv_in_b, ("sp", "fs"), axis=0, tiled=True),
        lax.all_gather(query_w, ("sp", "fs"), axis=0, tiled=True),
        lax.all_gather(key_w, ("sp", "fs"), axis=0, tiled=True),
        lax.all_gather(value_w, ("sp", "fs"), axis=0, tiled=True),
        lax.all_gather(out_gate_w, ("sp", "fs"), axis=0, tiled=True),
        lax.all_gather(pointwise_w, ("sp", "fs"), axis=0, tiled=True),
        lax.all_gather(gla_out_w, ("sp", "fs"), axis=0, tiled=True),
    )
    (
        conv_a_full,
        conv_b_full,
        query_full,
        key_full,
        value_full,
        gate_full,
        pointwise_full,
        gla_out_full,
    ) = collected
    tok_rows = inputs[0]
    token_count = tok_rows.shape[0]
    in_weights = (
        conv_a_full,
        conv_b_full,
        query_full,
        key_full,
        value_full,
        gate_full,
        forget_first_factor,
    )
    segment_values = lax.all_gather(tok_rows, "tp", axis=1, tiled=True).astype(jnp.float32)
    scaled = (segment_values * norm_gain).astype(jnp.bfloat16)
    sums = tuple(
        (jnp.dot(scaled, weight, preferred_element_type=jnp.float32) for weight in in_weights)
    )
    sums, squares = (sums, jnp.sum(segment_values * segment_values, axis=1))
    row_scale = lax.rsqrt(squares / norm_gain.shape[0] + 1e-06)[:, None]
    conv_a, conv_b, queries, keys, values, out_gate, low_rank = [
        (running * row_scale).astype(jnp.bfloat16) for running in sums
    ]
    gated = (conv_a.astype(jnp.float32) * jax.nn.sigmoid(conv_b.astype(jnp.float32))).astype(
        jnp.bfloat16
    )
    reach = conv_kernel.shape[0] - 1
    earlier = from_behind(gated[token_count - reach :], "sp", 1)
    extended = jnp.concatenate([earlier, gated], axis=0).astype(jnp.float32)
    tp_index = lax.axis_index("tp")
    channels = gated.shape[1]
    kernel = lax.dynamic_slice_in_dim(conv_kernel, tp_index * channels, channels, 1)
    convolved = jnp.zeros((token_count, channels), jnp.float32)
    for offset in range(reach + 1):
        convolved = convolved + kernel[offset] * extended[offset : offset + token_count]
    channel_sum, channel_squares = lax.psum(
        (jnp.sum(convolved, axis=1), jnp.sum(convolved * convolved, axis=1)), "tp"
    )
    total_channels = conv_gain.shape[0]
    average = channel_sum / total_channels
    spread_squared_mean = channel_squares / total_channels - average * average
    gain_part = lax.dynamic_slice_in_dim(conv_gain, tp_index * channels, channels)
    normed = (
        (convolved - average[:, None]) * lax.rsqrt(spread_squared_mean + 1e-05)[:, None] * gain_part
    )
    conv_act = jax.nn.silu(normed).astype(jnp.bfloat16)
    key_width = keys.shape[1]
    head_count = key_width // DK
    decay_part = lax.dynamic_slice_in_dim(decay_w, tp_index * key_width, key_width, 1)
    bias_part = lax.dynamic_slice_in_dim(decay_bias, tp_index * key_width, key_width)
    pre_decay = jnp.dot(low_rank, decay_part, preferred_element_type=jnp.float32) + bias_part
    log_decay = jax.nn.log_sigmoid(pre_decay) / 16.0 + decay_extra[0]
    block_count = token_count // BLOCK
    highest = lax.Precision.HIGHEST

    def split_blocks(array_operand, width):
        return array_operand.reshape(block_count, BLOCK, head_count, width).transpose(0, 2, 1, 3)

    q_blocks = split_blocks(queries.astype(jnp.float32), DK) * DK ** (-0.5)
    k_blocks = split_blocks(keys.astype(jnp.float32), DK)
    v_blocks = split_blocks(values.astype(jnp.float32), DV)
    prefix_running_sum = jnp.cumsum(split_blocks(log_decay, DK), axis=2)
    causal = jnp.tril(jnp.ones((BLOCK, BLOCK), dtype=bool))
    spread = prefix_running_sum[:, :, :, None, :] - prefix_running_sum[:, :, None, :, :]
    weights_in = jnp.exp(jnp.where(causal[:, :, None], spread, -jnp.inf))
    scores = jnp.einsum("nhid,nhjd,nhijd->nhij", q_blocks, k_blocks, weights_in, precision=highest)
    inner = jnp.einsum("nhij,nhjv->nhiv", scores, v_blocks, precision=highest)
    block_total = prefix_running_sum[:, :, -1]
    block_state = jnp.einsum(
        "nhjd,nhjv->nhdv",
        k_blocks * jnp.exp(block_total[:, :, None] - prefix_running_sum),
        v_blocks,
        precision=highest,
    )

    def advance(state, block_pair):
        decay_row, added_share_term = block_pair
        return (jnp.exp(decay_row)[..., None] * state + added_share_term, state)

    local_final, local_entering = lax.scan(
        advance, jnp.zeros((head_count, DK, DV), jnp.float32), (block_total, block_state)
    )
    device_total = jnp.sum(block_total, axis=0)
    totals = lax.all_gather(device_total[None], "sp", axis=0, tiled=True)
    running_totals = jnp.cumsum(totals, axis=0)
    sp_index = lax.axis_index("sp")
    before = lax.dynamic_index_in_dim(
        running_totals, sp_index, 0, False
    ) - lax.dynamic_index_in_dim(totals, sp_index, 0, False)
    piece = lax.all_gather(local_final[None], "sp", axis=0, tiled=True)
    number = piece.shape[0]
    anchor = jnp.arange(number, dtype=jnp.int32)
    exponent = jnp.where(
        (anchor < sp_index)[:, None, None], before[None] - running_totals, -jnp.inf
    )
    entering = jnp.einsum("nhd,nhdv->hdv", jnp.exp(exponent), piece, precision=highest)
    passed = jnp.exp(jnp.cumsum(block_total, axis=0) - block_total)
    entering_blocks = passed[..., None] * entering[None] + local_entering
    outer = jnp.einsum(
        "nhid,nhdv->nhiv",
        q_blocks * jnp.exp(prefix_running_sum),
        entering_blocks,
        precision=highest,
    )
    head_output = inner + outer
    normed_heads = (
        head_output
        * lax.rsqrt(jnp.mean(head_output * head_output, axis=-1, keepdims=True) + 1e-06)
        * head_gain
    )
    gla_rows = normed_heads.transpose(0, 2, 1, 3).reshape(token_count, head_count * DV)
    gla_act = (gla_rows * jax.nn.silu(out_gate.astype(jnp.float32))).astype(jnp.bfloat16)
    contract = (((1,), (1,)), ((), ()))
    conv_term = lax.dot_general(
        pointwise_full, conv_act, contract, preferred_element_type=jnp.float32
    )
    summed = lax.psum_scatter(
        (
            conv_term
            + lax.dot_general(gla_out_full, gla_act, contract, preferred_element_type=jnp.float32)
        ).astype(jnp.bfloat16),
        "tp",
        scatter_dimension=0,
        tiled=True,
    ).astype(jnp.float32)
    return (tok_rows.astype(jnp.float32) + summed.T).astype(jnp.bfloat16)[None]


def shards(*args):
    n_sp, n_tp = lax.axis_size("sp"), lax.axis_size("tp")
    head_count = args[5].shape[1] // DK
    whole_heads = head_count % n_sp == 0 and n_sp % n_tp == 0
    return by_heads(*args) if whole_heads else by_tokens(*args)


def solution(mesh):
    by_rows = P(("sp", "fs"), "tp")
    return jax.shard_map(
        shards,
        mesh=mesh,
        in_specs=(P("fs", "sp", "tp"), P())
        + (by_rows,) * 8
        + (P(), P(), P(), P("fs", "sp", "tp"), P(), P(), P()),
        out_specs=P("fs", "sp", "tp"),
        check_vma=False,
    )
```
